32 devices in a mesh: gr: 2 (over y), sp: 4 (over z), tp: 4 (over x, core).
Axes of the slice: x: 2, y: 2, z: 4, core: 2. Of those that a mesh axis runs over, the one named last changes fastest.
Arguments:
- tokens: bfloat16 [8, 768, 4096], P('gr', 'sp'), parts along dimension 0, may hold values from -50 to 50
- new_tokens: bfloat16 [8, 4096], P('gr'), parts along dimension 0, may hold values from -6 to 6
- in_gain: float32 [4096], replicated, may hold values from 0.1 to 1.9
- w_forget: bfloat16 [4096, 2048], P(None, 'tp'), may hold values from -0.09375 to 0.09375
- w_value: bfloat16 [4096, 2048], P(None, 'tp'), may hold values from -0.75 to 0.75
- gap: float32 [16, 128], P('tp'), may hold values from 0 to 0.06
- decay_shift: float32 [8, 768, 16], P('gr', 'sp', 'tp'), parts along dimension 0, may hold values from -3 to 0
- query: bfloat16 [8, 16, 128], P('gr', 'tp', 'sp'), parts along dimension 0, may hold values from -6 to 6
- out_gain: float32 [16, 128], P('tp'), may hold values from 0.1 to 1.9
Outputs:
- cache: bfloat16 [8, 16, 128, 128], P('gr', 'tp', 'sp'), parts along dimension 0
- read: float32 [8, 16, 128], P('gr', 'tp'), parts along dimension 0
The draws below stay inside these ranges and needn't reach their ends.
There are 2 independent parts, one for each index of `gr`. The reference program is written for one: setup_inputs(seed, part) draws one part's arguments, and reference() takes and returns one part's arrays. A program takes and returns all parts, laid end to end along the dimension named above; an argument that names none is the same for every part. Nothing has to cross between parts.
All inputs are finite; a program needn't handle non-finite values.
Results may differ from the reference program's by a relative error of at most 0.0065.
Values sent between devices are 32-bit elements; how exact they have to be, the bound alone decides.
A program may use at most 64 MiB of HBM per device.

```python
import math
import jax
import jax.numpy as jnp
from jax import lax

D = 4096
H = 16
DK = 128
DV = 128
SEQS = 4
SEG = 192
LEN = 768


def draw_tokens(key, part):
    sample_key, scale_key = jax.random.split(key, 2)
    sample = jnp.clip(jax.random.normal(sample_key, (SEQS, LEN, D)), -5.0, 5.0)
    scales = jnp.exp(jax.random.uniform(scale_key, (SEQS, LEN, 1), minval=0.0, maxval=math.log(10.0)))
    return (sample * scales).astype(jnp.bfloat16)


def draw_gap(key, part):
    order_key, slow_key, fast_key = jax.random.split(key, 3)
    ranking = jax.random.permutation(order_key, H)
    keep_count = H // 2
    slow_head = (ranking < keep_count)[:, None]
    slow_gap = jnp.exp(jax.random.uniform(slow_key, (H, DK), minval=math.log(0.2), maxval=math.log(0.8))) / LEN
    fast_gap = jnp.exp(jax.random.uniform(fast_key, (H, DK), minval=math.log(0.02), maxval=math.log(0.06)))
    return jnp.where(slow_head, slow_gap, fast_gap).astype(jnp.float32)


def draw_decay_shift(key, part):
    rate_random_key, spot_key, depth_key, closing_key = jax.random.split(key, 4)
    block_count = LEN // SEG
    low_rate, high_rate = (0.05, 0.5)
    rates = jnp.exp(jax.random.uniform(rate_random_key, (SEQS, block_count, 1, H), minval=math.log(low_rate), maxval=math.log(high_rate))) / LEN
    reference_floor = jnp.broadcast_to(rates, (SEQS, block_count, SEG, H)).reshape(SEQS, LEN, H)
    spots = jax.random.randint(spot_key, (SEQS, 2, H), 0, LEN)
    layer_depths = jax.random.uniform(depth_key, (SEQS, 2, H), minval=0.22, maxval=0.69)
    places = jnp.arange(LEN, dtype=jnp.int32)
    spike_hits = places[None, None, :, None] == spots[:, :, None, :]
    spike_events = jnp.sum(jnp.where(spike_hits, layer_depths[:, :, None, :], 0.0), axis=1)
    closing_depth = jax.random.uniform(closing_key, (SEQS, 1, H), minval=1.2, maxval=1.4)
    closing_rows = (places >= LEN - 3)[None, :, None]
    closing_events = jnp.where(closing_rows, closing_depth, 0.0)
    return (-reference_floor - spike_events - closing_events).astype(jnp.float32)


def levels(rng, dims, shards, smallest, largest):
    factor_of = 1.0
    for axis_at, shards_of in shards:
        draws = jax.random.uniform(jax.random.fold_in(jax.random.fold_in(rng, 6), axis_at), (shards_of,), jnp.float32, smallest / len(shards), largest / len(shards))
        factor_of = factor_of * jnp.repeat(jnp.exp(draws), dims[axis_at] // shards_of).reshape((-1,) + (1,) * (len(dims) - 1 - axis_at))
    return factor_of


def normal_values(stream_key, extent, scale, reach, cuts=(), kind=jnp.bfloat16):
    level = levels(stream_key, extent, cuts, -0.22, 0.18) if cuts else 1.0
    values = jax.random.normal(stream_key, extent, jnp.float32) * scale * level
    return jnp.minimum(jnp.maximum(values, -reach), reach).astype(kind)


def setup_inputs(seed: int = 0, part: int = 0) -> dict:
    streams_of = jax.random.split(jax.random.key(seed), 10)
    part_splits = jax.random.split(jax.random.fold_in(streams_of[9], part), 10)
    return {
        "tokens": draw_tokens(jax.random.fold_in(jax.random.fold_in(streams_of[9], part), 71), part),
        "new_tokens": normal_values(part_splits[1], (SEQS, D), 1.0, 6.0),
        "in_gain": jnp.clip(1.0 + 0.18 * jax.random.normal(streams_of[2], (D,), jnp.float32), 0.1, 1.9),
        "w_forget": normal_values(streams_of[3], (D, H * DK), D ** -0.5, 0.09375, ((1, 4),)),
        "w_value": normal_values(streams_of[4], (D, H * DV), (D // 64) ** -0.5, 0.75, ((1, 4),)),
        "gap": draw_gap(jax.random.fold_in(streams_of[9], 71), part),
        "decay_shift": draw_decay_shift(jax.random.fold_in(jax.random.fold_in(streams_of[9], part), 71), part),
        "query": normal_values(part_splits[7], (SEQS, H, DK), 1.0, 6.0, ((1, 4), (2, 4))),
        "out_gain": jnp.clip(1.0 + 0.18 * jax.random.normal(streams_of[8], (H, DV), jnp.float32), 0.1, 1.9),
    }


epsilon = 1e-06

def normalize(row_block, gain_row):
    widened = row_block.astype(jnp.float32)
    scaled = widened * lax.rsqrt(lax.optimization_barrier(jnp.mean(widened * widened, axis=-1, keepdims=True)) + epsilon)
    return (scaled * gain_row).astype(jnp.bfloat16)

def reference(tokens, new_tokens, in_gain, w_forget, w_value, gap, decay_shift, query, out_gain):
    block_count = LEN // SEG

    def one_prompt(inputs):
        seq_rows, decay_factor_row = inputs
        unit_norm_rows = normalize(seq_rows, in_gain)
        forget_pre = jnp.dot(unit_norm_rows, w_forget, preferred_element_type=jnp.float32).reshape(LEN, H, DK)
        values = lax.optimization_barrier(jnp.dot(unit_norm_rows, w_value, preferred_element_type=jnp.float32).astype(jnp.bfloat16))
        values = values.astype(jnp.float32).reshape(block_count, SEG, H, DV)
        key_gate = gap * jax.nn.sigmoid(-forget_pre)
        forget_logarithm = jnp.log1p(-key_gate) + decay_factor_row[:, :, None]
        blocks = forget_logarithm.reshape(block_count, SEG, H, DK)
        totals = lax.optimization_barrier(jnp.sum(blocks, axis=1))
        within = totals[:, None] - jnp.cumsum(blocks, axis=1)
        weights = lax.optimization_barrier((key_gate.reshape(block_count, SEG, H, DK) * jnp.exp(within)).astype(jnp.bfloat16))
        pieces = jnp.einsum('gthi,gthj->ghij', weights.astype(jnp.float32), values)
        later_sum = jnp.cumsum(totals[::-1], axis=0)[::-1] - totals
        return lax.optimization_barrier(jnp.sum(jnp.exp(later_sum)[..., None] * pieces, axis=0))
    full_state = lax.map(one_prompt, (tokens, decay_shift))
    cache = full_state.astype(jnp.bfloat16)
    normed_new = normalize(new_tokens, in_gain)
    new_pre = jnp.dot(normed_new, w_forget, preferred_element_type=jnp.float32).reshape(SEQS, H, DK)
    new_key = gap * jax.nn.sigmoid(-new_pre)
    new_values = lax.optimization_barrier(jnp.dot(normed_new, w_value, preferred_element_type=jnp.float32).astype(jnp.bfloat16))
    new_values = new_values.astype(jnp.float32).reshape(SEQS, H, DV)
    updated = (1.0 - new_key)[..., None] * full_state + new_key[..., None] * new_values[:, :, None, :]
    read_raw = jnp.einsum('shi,shij->shj', query.astype(jnp.float32), updated, precision=lax.Precision.HIGHEST)
    read = read_raw * lax.rsqrt(lax.optimization_barrier(jnp.mean(read_raw * read_raw, axis=-1, keepdims=True)) + epsilon) * out_gain
    return (cache, read)
```

```python
import functools

import jax
import jax.numpy as jnp
from jax import lax
from jax.experimental import pallas as pl
from jax.experimental.pallas import tpu as pltpu
from jax.sharding import PartitionSpec as P

epsilon = 1e-06
LAG = 1
ROWS = 16
TOKEN_CUTS = 4
WEIGHT_CUTS = 2
MESH = pl.DeviceIdType.MESH


def normalize(rows, gain):
    wide = rows.astype(jnp.float32)
    scaled = wide * lax.rsqrt(jnp.mean(wide * wide, axis=-1, keepdims=True) + epsilon)
    return (scaled * gain).astype(jnp.bfloat16)


def column(row, size):
    return jnp.broadcast_to(row, (size, size)).T


def kernel(
    tokens, new_tokens, in_gain, w_forget, w_value, gap, shift, query, out_gain,
    cache, read,
    tok_s, w_s, new_s, gain_s, gap_s, shift_s, query_s, og_s,
    normed, later, pieces, grow, grow_t, from_left, from_right,
    total_s, total_out, total_in, act, extra, spread, parts,
    tok_sem, w_sem, small_sem,
    f_send, f_recv, b_send, b_recv, t_send, t_recv, r_send, r_recv,
):
    g = lax.axis_index("sp")
    n = lax.axis_size("sp")
    seqs, seg, width = tok_s.shape
    wide_blocks, _, cols = w_s.shape
    heads, keys = gap_s.shape
    per = heads // wide_blocks
    vals = og_s.shape[1]
    rows = keys // n
    blocks = seqs * wide_blocks
    half = per * keys

    def tok_copy(s, i):
        part = pl.ds(i * (seg // TOKEN_CUTS), seg // TOKEN_CUTS)
        return pltpu.make_async_copy(tokens.at[s, part], tok_s.at[s, part], tok_sem.at[s, i])

    def w_copy(k, which, i):
        part = pl.ds(i * (width // WEIGHT_CUTS), width // WEIGHT_CUTS)
        source = (w_forget, w_value)[which]
        at = pl.multiple_of(k * half, half)
        return pltpu.make_async_copy(
            source.at[part, pl.ds(at, half)],
            w_s.at[k, part, pl.ds(which * half, half)],
            w_sem.at[k, which, i],
        )

    smalls = [
        pltpu.make_async_copy(a, b, small_sem.at[i])
        for i, (a, b) in enumerate(
            (
                (in_gain, gain_s), (gap, gap_s), (shift, shift_s),
                (new_tokens, new_s), (query, query_s), (out_gain, og_s),
            )
        )
    ]
    smalls[0].start()
    for i in range(TOKEN_CUTS):
        tok_copy(0, i).start()
    for k in range(wide_blocks):
        for i in range(WEIGHT_CUTS):
            for which in range(2):
                w_copy(k, which, i).start()
        if k == 0:
            for copy in smalls[1:3]:
                copy.start()
    for s in range(1, seqs):
        for i in range(TOKEN_CUTS):
            tok_copy(s, i).start()
    for copy in smalls[3:]:
        copy.start()

    barrier = pltpu.get_barrier_semaphore()
    for k in range(1, n):
        pl.semaphore_signal(
            barrier, inc=1, device_id={"sp": lax.rem(g + k, n)}, device_id_type=MESH
        )

    place = lax.broadcasted_iota(jnp.int32, (seg, seg), 0)
    other = lax.broadcasted_iota(jnp.int32, (seg, seg), 1)
    later[...] = jnp.where(other > place, 1.0, 0.0).astype(jnp.bfloat16)
    smalls[0].wait()

    right, left = lax.rem(g + 1, n), lax.rem(g + n - 1, n)

    def forward(b, d):
        return pltpu.make_async_remote_copy(
            src_ref=pieces.at[b, d], dst_ref=from_left.at[b, d],
            send_sem=f_send.at[b, d], recv_sem=f_recv.at[b, d],
            device_id={"sp": right}, device_id_type=MESH,
        )

    def backward(b, d):
        return pltpu.make_async_remote_copy(
            src_ref=pieces.at[b, d], dst_ref=from_right.at[b, d],
            send_sem=b_send.at[b, d], recv_sem=b_recv.at[b, d],
            device_id={"sp": left}, device_id_type=MESH,
        )

    def carried(b):
        return pltpu.make_async_remote_copy(
            src_ref=total_out.at[b], dst_ref=total_in.at[b],
            send_sem=t_send.at[b], recv_sem=t_recv.at[b],
            device_id={"sp": left}, device_id_type=MESH,
        )

    def loop(low, high, body):
        lax.fori_loop(low, high, lambda i, c: (body(i), c)[1], 0)

    def scatter(ref, b, j, square):
        for d in range(n):
            ref[b, d, j] = square[d * rows : (d + 1) * rows]

    def compute(b):
        s, k = b // wide_blocks, b % wide_blocks

        @pl.when(k == 0)
        def _():
            for i in range(TOKEN_CUTS):
                tok_copy(s, i).wait()

            def rows_of(i):
                at = pl.ds(pl.multiple_of(i * ROWS, ROWS), ROWS)
                normed[at, :] = normalize(tok_s[s, at, :], gain_s[...])

            loop(0, seg // ROWS, rows_of)

        @pl.when(s == 0)
        def _():
            for i in range(WEIGHT_CUTS):
                for which in range(2):
                    w_copy(k, which, i).wait()

        @pl.when(b == 0)
        def _():
            for copy in smalls[1:3]:
                copy.wait()

        both = jnp.dot(normed[...], w_s[k], preferred_element_type=jnp.float32)
        forget_pre = both[:, :half]
        values = both[:, half:].astype(jnp.bfloat16)
        shifts = shift_s[s]
        lane = lax.broadcasted_iota(jnp.int32, shifts.shape, 1)
        gains, moves = [], []
        for j in range(per):
            gains.append(gap_s[pl.ds(k * per + j, 1), :])
            one = jnp.sum(jnp.where(lane == k * per + j, shifts, 0.0), axis=1, keepdims=True)
            moves.append(jnp.broadcast_to(one, (seg, keys)))
        key_gate = jnp.concatenate(gains, axis=1) * jax.nn.sigmoid(-forget_pre)
        log_forget = jnp.log1p(-key_gate) + jnp.concatenate(moves, axis=1)
        high = log_forget.astype(jnp.bfloat16)
        rest = log_forget - high.astype(jnp.float32)
        mid = rest.astype(jnp.bfloat16)
        low = (rest - mid.astype(jnp.float32)).astype(jnp.bfloat16)
        sums = jnp.dot(
            later[...], jnp.concatenate([high, mid, low], axis=1),
            preferred_element_type=jnp.float32,
        )
        within = sums[:, :half] + (sums[:, half : 2 * half] + sums[:, 2 * half :])
        totals = jnp.sum(log_forget, axis=0, keepdims=True)
        weights = (key_gate * jnp.exp(within)).astype(jnp.bfloat16)
        total_s[b] = totals
        for j in range(per):
            at = slice(j * keys, (j + 1) * keys)
            piece = lax.dot_general(
                weights[:, at], values[:, j * vals : (j + 1) * vals],
                (((0,), (0,)), ((), ())), preferred_element_type=jnp.float32,
            )
            scatter(pieces, b, j, piece)
            scatter(grow, b, j, jnp.exp(column(totals[:, at], keys)))

    def send_first(b):
        @pl.when(g == 0)
        def _():
            loop(0, n - 1, lambda i: forward(b, n - 1 - i).start())

        @pl.when(g == n - 1)
        def _():
            total_out[b] = total_s[b]
            carried(b).start()
            loop(0, n - 1, lambda d: backward(b, d).start())

    def service(b):
        @pl.when(g < n - 1)
        def _():
            carried(b).wait_recv()
            arrived = total_in[b]
            for j in range(per):
                scatter(grow_t, b, j, jnp.exp(column(arrived[:, j * keys : (j + 1) * keys], keys)))

        @pl.when((g > 0) & (g < n - 1))
        def _():
            total_out[b] = total_in[b] + total_s[b]
            carried(b).start()

            def on_right(i):
                d = n - 1 - i
                forward(b, d).wait_recv()
                pieces[b, d] = grow[b, d] * from_left[b, d] + pieces[b, d]
                forward(b, d).start()

            def on_left(d):
                backward(b, d).wait_recv()
                pieces[b, d] = from_right[b, d] + grow_t[b, d] * pieces[b, d]
                backward(b, d).start()

            loop(0, n - 1 - g, on_right)
            loop(0, g, on_left)

    def step(b):
        compute(b)

        @pl.when(b == 0)
        def _():
            pl.semaphore_wait(barrier, n - 1)

        send_first(b)

        @pl.when(b >= LAG)
        def _():
            service(b - LAG)

    loop(0, blocks, step)
    for b in range(blocks - LAG, blocks):
        service(b)

    for copy in smalls[3:]:
        copy.wait()
    new_normed = normalize(new_s[...], gain_s[...])
    new_normed = jnp.concatenate(
        [new_normed, jnp.zeros((16 - seqs, width), jnp.bfloat16)], axis=0
    ) if seqs < 16 else new_normed
    pick = (
        lax.broadcasted_iota(jnp.int32, (rows, keys), 1)
        == lax.broadcasted_iota(jnp.int32, (rows, keys), 0) + g * rows
    )
    pick = jnp.where(pick, 1.0, 0.0).astype(jnp.bfloat16)
    placed = [
        jnp.dot(query_s[s], pick, preferred_element_type=jnp.float32) for s in range(seqs)
    ]
    for k in range(wide_blocks):
        both = jnp.dot(new_normed, w_s[k], preferred_element_type=jnp.float32)
        for j in range(per):
            h = k * per + j
            new_key = gap_s[h : h + 1, :] * jax.nn.sigmoid(-both[:seqs, j * keys : (j + 1) * keys])
            new_value = both[:seqs, half + j * vals : half + (j + 1) * vals]
            new_value = new_value.astype(jnp.bfloat16).astype(jnp.float32)
            for s in range(seqs):
                q = placed[s][h : h + 1, :]
                key_row = new_key[s : s + 1, :]
                square = column(q * (1.0 - key_row), keys)
                for d in range(n):
                    spread[d] = square[d * rows : (d + 1) * rows]
                b = s * wide_blocks + k
                act[b, j] = spread[g]
                weight = jnp.sum(q * key_row, axis=1, keepdims=True)
                extra[b * per + j : b * per + j + 1, :] = weight * new_value[s : s + 1, :]

    def finish(b):
        @pl.when(g > 0)
        def _():
            forward(b, g).wait_recv()
            pieces[b, g] = pieces[b, g] + grow[b, g] * from_left[b, g]

        @pl.when(g < n - 1)
        def _():
            backward(b, g).wait_recv()
            pieces[b, g] = from_right[b, g] + grow_t[b, g] * pieces[b, g]

    for b in range(blocks):
        finish(b)
        s, k = b // wide_blocks, b % wide_blocks
        for j in range(per):
            state = pieces[b, g, j]
            cache[s, k * per + j] = state.astype(jnp.bfloat16)
            at = b * per + j
            parts[g, at : at + 1, :] = (
                jnp.sum(act[b, j] * state, axis=0, keepdims=True) + extra[at : at + 1, :]
            )

    def share(k):
        to = lax.rem(g + k, n)
        return pltpu.make_async_remote_copy(
            src_ref=parts.at[g], dst_ref=parts.at[g],
            send_sem=r_send.at[k], recv_sem=r_recv.at[k],
            device_id={"sp": to}, device_id_type=MESH,
        )

    def arrival(k):
        source = lax.rem(g + n - k, n)
        return pltpu.make_async_remote_copy(
            src_ref=parts.at[source], dst_ref=parts.at[source],
            send_sem=r_send.at[k], recv_sem=r_recv.at[k],
            device_id={"sp": source}, device_id_type=MESH,
        )

    loop(1, n, lambda k: share(k).start())

    def drain(b):
        @pl.when(g < n - 1)
        def _():
            loop(g + 1, n, lambda d: forward(b, d).wait_send())

        @pl.when(g > 0)
        def _():
            carried(b).wait_send()
            loop(0, g, lambda d: backward(b, d).wait_send())

    loop(0, blocks, drain)
    loop(1, n, lambda k: arrival(k).wait_recv())
    raw = parts[0]
    for d in range(1, n):
        raw = raw + parts[d]
    scaled = raw * lax.rsqrt(jnp.mean(raw * raw, axis=-1, keepdims=True) + epsilon)
    for s in range(seqs):
        read[s] = scaled[s * heads : (s + 1) * heads] * og_s[...]
    loop(1, n, lambda k: share(k).wait_send())


def local(tokens, new_tokens, in_gain, w_forget, w_value, gap, decay_shift, query, out_gain):
    seqs, seg, width = tokens.shape
    heads, keys = gap.shape
    vals = out_gain.shape[1]
    n = lax.axis_size("sp")
    rows = keys // n
    per = 2 if heads % 2 == 0 else 1
    wide_blocks = heads // per
    blocks = seqs * wide_blocks
    f32, bf16 = jnp.float32, jnp.bfloat16
    dma = pltpu.SemaphoreType.DMA
    grid = (blocks, n, per, rows, vals)
    return pl.pallas_call(
        kernel,
        out_shape=(
            jax.ShapeDtypeStruct((seqs, heads, rows, vals), bf16),
            jax.ShapeDtypeStruct((seqs, heads, vals), f32),
        ),
        in_specs=[pl.BlockSpec(memory_space=pl.ANY)] * 9,
        out_specs=(pl.BlockSpec(memory_space=pltpu.VMEM),) * 2,
        scratch_shapes=[
            pltpu.VMEM((seqs, seg, width), bf16),
            pltpu.VMEM((wide_blocks, width, per * (keys + vals)), bf16),
            pltpu.VMEM((seqs, width), bf16),
            pltpu.VMEM((1, width), f32),
            pltpu.VMEM((heads, keys), f32),
            pltpu.VMEM((seqs, seg, heads), f32),
            pltpu.VMEM((seqs, heads, rows), bf16),
            pltpu.VMEM((heads, vals), f32),
            pltpu.VMEM((seg, width), bf16),
            pltpu.VMEM((seg, seg), bf16),
            pltpu.VMEM(grid, f32),
            pltpu.VMEM(grid, f32),
            pltpu.VMEM(grid, f32),
            pltpu.VMEM(grid, f32),
            pltpu.VMEM(grid, f32),
            pltpu.VMEM((blocks, 1, per * keys), f32),
            pltpu.VMEM((blocks, 1, per * keys), f32),
            pltpu.VMEM((blocks, 1, per * keys), f32),
            pltpu.VMEM((blocks, per, rows, vals), f32),
            pltpu.VMEM((blocks * per, vals), f32),
            pltpu.VMEM((n, rows, vals), f32),
            pltpu.VMEM((n, blocks * per, vals), f32),
            dma((seqs, TOKEN_CUTS)),
            dma((wide_blocks, 2, WEIGHT_CUTS)),
            dma((6,)),
            dma((blocks, n)),
            dma((blocks, n)),
            dma((blocks, n)),
            dma((blocks, n)),
            dma((blocks,)),
            dma((blocks,)),
            dma((n,)),
            dma((n,)),
        ],
        compiler_params=pltpu.CompilerParams(
            collective_id=0, has_side_effects=True, vmem_limit_bytes=60 * 1024 * 1024
        ),
        name="recurrence",
    )(
        tokens, new_tokens, in_gain.reshape(1, width), w_forget, w_value, gap,
        decay_shift, query, out_gain,
    )


def solution(mesh):
    return jax.shard_map(
        local,
        mesh=mesh,
        in_specs=(
            P("gr", "sp", None),
            P("gr", None),
            P(),
            P(None, "tp"),
            P(None, "tp"),
            P("tp", None),
            P("gr", "sp", "tp"),
            P("gr", "tp", "sp"),
            P("tp", None),
        ),
        out_specs=(P("gr", "tp", "sp", None), P("gr", "tp", None)),
        check_vma=False,
    )
```

```python
import functools

import jax
import jax.numpy as jnp
from jax import lax
from jax.experimental import pallas as pl
from jax.experimental.pallas import tpu as pltpu
from jax.sharding import PartitionSpec as P

epsilon = 1e-06
ROWS = 16
TOKEN_CUTS = 4
WEIGHT_CUTS = 2
MESH = pl.DeviceIdType.MESH


def normalize(rows, gain):
    wide = rows.astype(jnp.float32)
    scaled = wide * lax.rsqrt(jnp.mean(wide * wide, axis=-1, keepdims=True) + epsilon)
    return (scaled * gain).astype(jnp.bfloat16)


def column(row, size):
    return jnp.broadcast_to(row, (size, size)).T


def kernel(
    tokens, new_tokens, in_gain, w_forget, w_value, gap, shift, query, out_gain,
    cache, read,
    tok_s, w_s, new_s, gain_s, gap_s, shift_s, query_s, og_s,
    normed, later, pieces, grow, grow_t, from_left, from_right,
    total_s, total_out, total_in, act, extra, spread, parts,
    tok_sem, w_sem, small_sem,
    f_send, f_recv, b_send, b_recv, t_send, t_recv, r_send, r_recv,
):
    g = lax.axis_index("sp")
    n = lax.axis_size("sp")
    seqs, seg, width = tok_s.shape
    wide_blocks, _, cols = w_s.shape
    heads, keys = gap_s.shape
    per = heads // wide_blocks
    vals = og_s.shape[1]
    rows = keys // n
    blocks = seqs * wide_blocks
    half = per * keys

    def tok_copy(s, i):
        part = pl.ds(i * (seg // TOKEN_CUTS), seg // TOKEN_CUTS)
        return pltpu.make_async_copy(tokens.at[s, part], tok_s.at[s, part], tok_sem.at[s, i])

    def w_copy(k, which, i):
        part = pl.ds(i * (width // WEIGHT_CUTS), width // WEIGHT_CUTS)
        source = (w_forget, w_value)[which]
        at = pl.multiple_of(k * half, half)
        return pltpu.make_async_copy(
            source.at[part, pl.ds(at, half)],
            w_s.at[k, part, pl.ds(which * half, half)],
            w_sem.at[k, which, i],
        )

    smalls = [
        pltpu.make_async_copy(a, b, small_sem.at[i])
        for i, (a, b) in enumerate(
            (
                (in_gain, gain_s), (gap, gap_s), (shift, shift_s),
                (new_tokens, new_s), (query, query_s), (out_gain, og_s),
            )
        )
    ]
    smalls[0].start()
    for i in range(TOKEN_CUTS):
        tok_copy(0, i).start()
    for k in range(wide_blocks):
        for i in range(WEIGHT_CUTS):
            for which in range(2):
                w_copy(k, which, i).start()
        if k == 0:
            for copy in smalls[1:3]:
                copy.start()
    for s in range(1, seqs):
        for i in range(TOKEN_CUTS):
            tok_copy(s, i).start()
    for copy in smalls[3:]:
        copy.start()

    barrier = pltpu.get_barrier_semaphore()
    for k in range(1, n):
        pl.semaphore_signal(
            barrier, inc=1, device_id={"sp": lax.rem(g + k, n)}, device_id_type=MESH
        )

    place = lax.broadcasted_iota(jnp.int32, (seg, seg), 0)
    other = lax.broadcasted_iota(jnp.int32, (seg, seg), 1)
    later[...] = jnp.where(other > place, 1.0, 0.0).astype(jnp.bfloat16)
    smalls[0].wait()

    right, left = lax.rem(g + 1, n), lax.rem(g + n - 1, n)

    def forward(b, d):
        return pltpu.make_async_remote_copy(
            src_ref=pieces.at[b, d], dst_ref=from_left.at[b, d],
            send_sem=f_send.at[b, d], recv_sem=f_recv.at[b, d],
            device_id={"sp": right}, device_id_type=MESH,
        )

    def backward(b, d):
        return pltpu.make_async_remote_copy(
            src_ref=pieces.at[b, d], dst_ref=from_right.at[b, d],
            send_sem=b_send.at[b, d], recv_sem=b_recv.at[b, d],
            device_id={"sp": left}, device_id_type=MESH,
        )

    def carried(b):
        return pltpu.make_async_remote_copy(
            src_ref=total_out.at[b], dst_ref=total_in.at[b],
            send_sem=t_send.at[b], recv_sem=t_recv.at[b],
            device_id={"sp": left}, device_id_type=MESH,
        )

    def loop(low, high, body):
        lax.fori_loop(low, high, lambda i, c: (body(i), c)[1], 0)

    def scatter(ref, b, j, square):
        for d in range(n):
            ref[b, d, j] = square[d * rows : (d + 1) * rows]

    def compute(b):
        s, k = b // wide_blocks, b % wide_blocks

        @pl.when(k == 0)
        def _():
            for i in range(TOKEN_CUTS):
                tok_copy(s, i).wait()

            def rows_of(i):
                at = pl.ds(pl.multiple_of(i * ROWS, ROWS), ROWS)
                normed[at, :] = normalize(tok_s[s, at, :], gain_s[...])

            loop(0, seg // ROWS, rows_of)

        @pl.when(s == 0)
        def _():
            for i in range(WEIGHT_CUTS):
                for which in range(2):
                    w_copy(k, which, i).wait()

        @pl.when(b == 0)
        def _():
            for copy in smalls[1:3]:
                copy.wait()

        both = jnp.dot(normed[...], w_s[k], preferred_element_type=jnp.float32)
        forget_pre = both[:, :half]
        values = both[:, half:].astype(jnp.bfloat16)
        chosen = (
            lax.broadcasted_iota(jnp.int32, (heads, half), 0)
            == lax.broadcasted_iota(jnp.int32, (heads, half), 1) // keys + k * per
        )
        moves = lax.dot_general(
            shift_s[s], jnp.where(chosen, 1.0, 0.0), (((0,), (0,)), ((), ())),
            precision=lax.Precision.HIGHEST, preferred_element_type=jnp.float32,
        )
        gains = [gap_s[pl.ds(k * per + j, 1), :] for j in range(per)]
        key_gate = jnp.concatenate(gains, axis=1) * jax.nn.sigmoid(-forget_pre)
        log_forget = jnp.log1p(-key_gate) + moves
        high = log_forget.astype(jnp.bfloat16)
        rest = log_forget - high.astype(jnp.float32)
        mid = rest.astype(jnp.bfloat16)
        low = (rest - mid.astype(jnp.float32)).astype(jnp.bfloat16)
        sums = jnp.dot(
            later[...], jnp.concatenate([high, mid, low], axis=1),
            preferred_element_type=jnp.float32,
        )
        within = sums[:, :half] + (sums[:, half : 2 * half] + sums[:, 2 * half :])
        totals = jnp.sum(log_forget, axis=0, keepdims=True)
        weights = (key_gate * jnp.exp(within)).astype(jnp.bfloat16)
        total_s[b] = totals
        for j in range(per):
            at = slice(j * keys, (j + 1) * keys)
            piece = lax.dot_general(
                weights[:, at], values[:, j * vals : (j + 1) * vals],
                (((0,), (0,)), ((), ())), preferred_element_type=jnp.float32,
            )
            scatter(pieces, b, j, piece)
            scatter(grow, b, j, jnp.exp(column(totals[:, at], keys)))

    def send_first(b):
        @pl.when(g == 0)
        def _():
            loop(0, n - 1, lambda i: forward(b, n - 1 - i).start())

        @pl.when(g == n - 1)
        def _():
            total_out[b] = total_s[b]
            carried(b).start()
            loop(0, n - 1, lambda d: backward(b, d).start())

    def to_right(b):
        def each(i):
            d = n - 1 - i
            forward(b, d).wait_recv()
            pieces[b, d] = grow[b, d] * from_left[b, d] + pieces[b, d]
            forward(b, d).start()

        loop(0, n - 1 - g, each)

    def to_left(b):
        carried(b).wait_recv()
        arrived = total_in[b]
        for j in range(per):
            scatter(grow_t, b, j, jnp.exp(column(arrived[:, j * keys : (j + 1) * keys], keys)))

        def each(d):
            backward(b, d).wait_recv()
            pieces[b, d] = from_right[b, d] + grow_t[b, d] * pieces[b, d]
            backward(b, d).start()

        @pl.when(g > 0)
        def _():
            total_out[b] = total_in[b] + total_s[b]
            carried(b).start()
            loop(0, g, each)

    def serve(t):
        right_b = t - g - 1
        left_b = t - n + g

        @pl.when((g > 0) & (g < n - 1) & (right_b >= 0) & (right_b < blocks))
        def _():
            to_right(right_b)

        @pl.when((g < n - 1) & (left_b >= 0) & (left_b < blocks))
        def _():
            to_left(left_b)

    def step(b):
        compute(b)

        @pl.when(b == 0)
        def _():
            pl.semaphore_wait(barrier, n - 1)

        send_first(b)
        serve(b)

    loop(0, blocks, step)
    serve(blocks)
    for copy in smalls[3:]:
        copy.wait()
    new_normed = normalize(new_s[...], gain_s[...])
    new_normed = jnp.concatenate(
        [new_normed, jnp.zeros((16 - seqs, width), jnp.bfloat16)], axis=0
    ) if seqs < 16 else new_normed
    pick = (
        lax.broadcasted_iota(jnp.int32, (rows, keys), 1)
        == lax.broadcasted_iota(jnp.int32, (rows, keys), 0) + g * rows
    )
    pick = jnp.where(pick, 1.0, 0.0).astype(jnp.bfloat16)
    placed = [
        jnp.dot(query_s[s], pick, preferred_element_type=jnp.float32) for s in range(seqs)
    ]
    for k in range(wide_blocks):
        both = jnp.dot(new_normed, w_s[k], preferred_element_type=jnp.float32)
        for j in range(per):
            h = k * per + j
            new_key = gap_s[h : h + 1, :] * jax.nn.sigmoid(-both[:seqs, j * keys : (j + 1) * keys])
            new_value = both[:seqs, half + j * vals : half + (j + 1) * vals]
            new_value = new_value.astype(jnp.bfloat16).astype(jnp.float32)
            for s in range(seqs):
                q = placed[s][h : h + 1, :]
                key_row = new_key[s : s + 1, :]
                square = column(q * (1.0 - key_row), keys)
                for d in range(n):
                    spread[d] = square[d * rows : (d + 1) * rows]
                b = s * wide_blocks + k
                act[b, j] = spread[g]
                weight = jnp.sum(q * key_row, axis=1, keepdims=True)
                extra[b * per + j : b * per + j + 1, :] = weight * new_value[s : s + 1, :]

    loop(blocks + 1, blocks + n, serve)

    def finish(b):
        @pl.when(g > 0)
        def _():
            forward(b, g).wait_recv()
            pieces[b, g] = pieces[b, g] + grow[b, g] * from_left[b, g]

        @pl.when(g < n - 1)
        def _():
            backward(b, g).wait_recv()
            pieces[b, g] = from_right[b, g] + grow_t[b, g] * pieces[b, g]

    for b in range(blocks):
        finish(b)
        s, k = b // wide_blocks, b % wide_blocks
        for j in range(per):
            state = pieces[b, g, j]
            cache[s, k * per + j] = state.astype(jnp.bfloat16)
            at = b * per + j
            parts[g, at : at + 1, :] = (
                jnp.sum(act[b, j] * state, axis=0, keepdims=True) + extra[at : at + 1, :]
            )

    def share(k):
        to = lax.rem(g + k, n)
        return pltpu.make_async_remote_copy(
            src_ref=parts.at[g], dst_ref=parts.at[g],
            send_sem=r_send.at[k], recv_sem=r_recv.at[k],
            device_id={"sp": to}, device_id_type=MESH,
        )

    def arrival(k):
        source = lax.rem(g + n - k, n)
        return pltpu.make_async_remote_copy(
            src_ref=parts.at[source], dst_ref=parts.at[source],
            send_sem=r_send.at[k], recv_sem=r_recv.at[k],
            device_id={"sp": source}, device_id_type=MESH,
        )

    loop(1, n, lambda k: share(k).start())

    def drain(b):
        @pl.when(g < n - 1)
        def _():
            loop(g + 1, n, lambda d: forward(b, d).wait_send())

        @pl.when(g > 0)
        def _():
            carried(b).wait_send()
            loop(0, g, lambda d: backward(b, d).wait_send())

    loop(0, blocks, drain)
    loop(1, n, lambda k: arrival(k).wait_recv())
    raw = parts[0]
    for d in range(1, n):
        raw = raw + parts[d]
    scaled = raw * lax.rsqrt(jnp.mean(raw * raw, axis=-1, keepdims=True) + epsilon)
    for s in range(seqs):
        read[s] = scaled[s * heads : (s + 1) * heads] * og_s[...]
    loop(1, n, lambda k: share(k).wait_send())


def local(tokens, new_tokens, in_gain, w_forget, w_value, gap, decay_shift, query, out_gain):
    seqs, seg, width = tokens.shape
    heads, keys = gap.shape
    vals = out_gain.shape[1]
    n = lax.axis_size("sp")
    rows = keys // n
    per = 2 if heads % 2 == 0 else 1
    wide_blocks = heads // per
    blocks = seqs * wide_blocks
    f32, bf16 = jnp.float32, jnp.bfloat16
    dma = pltpu.SemaphoreType.DMA
    grid = (blocks, n, per, rows, vals)
    return pl.pallas_call(
        kernel,
        out_shape=(
            jax.ShapeDtypeStruct((seqs, heads, rows, vals), bf16),
            jax.ShapeDtypeStruct((seqs, heads, vals), f32),
        ),
        in_specs=[pl.BlockSpec(memory_space=pl.ANY)] * 9,
        out_specs=(pl.BlockSpec(memory_space=pltpu.VMEM),) * 2,
        scratch_shapes=[
            pltpu.VMEM((seqs, seg, width), bf16),
            pltpu.VMEM((wide_blocks, width, per * (keys + vals)), bf16),
            pltpu.VMEM((seqs, width), bf16),
            pltpu.VMEM((1, width), f32),
            pltpu.VMEM((heads, keys), f32),
            pltpu.VMEM((seqs, heads, seg), f32),
            pltpu.VMEM((seqs, heads, rows), bf16),
            pltpu.VMEM((heads, vals), f32),
            pltpu.VMEM((seg, width), bf16),
            pltpu.VMEM((seg, seg), bf16),
            pltpu.VMEM(grid, f32),
            pltpu.VMEM(grid, f32),
            pltpu.VMEM(grid, f32),
            pltpu.VMEM(grid, f32),
            pltpu.VMEM(grid, f32),
            pltpu.VMEM((blocks, 1, per * keys), f32),
            pltpu.VMEM((blocks, 1, per * keys), f32),
            pltpu.VMEM((blocks, 1, per * keys), f32),
            pltpu.VMEM((blocks, per, rows, vals), f32),
            pltpu.VMEM((blocks * per, vals), f32),
            pltpu.VMEM((n, rows, vals), f32),
            pltpu.VMEM((n, blocks * per, vals), f32),
            dma((seqs, TOKEN_CUTS)),
            dma((wide_blocks, 2, WEIGHT_CUTS)),
            dma((6,)),
            dma((blocks, n)),
            dma((blocks, n)),
            dma((blocks, n)),
            dma((blocks, n)),
            dma((blocks,)),
            dma((blocks,)),
            dma((n,)),
            dma((n,)),
        ],
        compiler_params=pltpu.CompilerParams(
            collective_id=0, has_side_effects=True, vmem_limit_bytes=60 * 1024 * 1024
        ),
        name="recurrence",
    )(
        tokens, new_tokens, in_gain.reshape(1, width), w_forget, w_value, gap,
        decay_shift.transpose(0, 2, 1), query, out_gain,
    )


def solution(mesh):
    return jax.shard_map(
        local,
        mesh=mesh,
        in_specs=(
            P("gr", "sp", None),
            P("gr", None),
            P(),
            P(None, "tp"),
            P(None, "tp"),
            P("tp", None),
            P("gr", "sp", "tp"),
            P("gr", "tp", "sp"),
            P("tp", None),
        ),
        out_specs=(P("gr", "tp", "sp", None), P("gr", "tp", None)),
        check_vma=False,
    )
```
